32 devices in a mesh: gr: 2 (over x), sp: 8 (over z, y), tp: 2 (over core).
Axes of the slice: x: 2, y: 2, z: 4, core: 2. Of those that a mesh axis runs over, the one named last changes fastest.
Arguments:
- tokens: bfloat16 [2, 2, 6144, 2048], P('gr', 'tp', 'sp'), may hold values from -6 to 6
- key_weight: bfloat16 [2048, 2048], replicated, may hold values from -0.125 to 0.125
- value_weight: bfloat16 [2048, 2048], replicated, may hold values from -0.125 to 0.125
- cum_gate: float32 [2, 32, 2, 6144], P('gr', None, 'tp', 'sp'), may hold values from -12588 to 0, as said below
- query: bfloat16 [2, 32, 64], P('gr', 'sp'), may hold values from -12 to 12
Outputs:
- kv_cache: bfloat16 [2, 32, 12288, 128], P('gr', 'sp', 'tp')
- gate_cache: float32 [2, 32, 12288], P('gr', 'sp', 'tp')
- read: bfloat16 [2, 32, 64], P('gr', 'sp')
The draws below stay inside these ranges and needn't reach their ends.
Inputs may be any that keep to these rules, and one draw needn't show every extreme that they name: `cum_gate`: each head's entries never rise along the positions.
All inputs are finite; a program needn't handle non-finite values.
Results may differ from the reference program's by a relative error of at most 0.012.
Values may be sent and summed in bfloat16 or wider, within the bound.
A program may use at most 128 MiB of HBM per device.

```python
import jax
import jax.numpy as jnp

D = 2048
HEADS = 32
HD = 64
TOK_DEV = 768
SPAN = 6144
LEN = 12288
BATCH = 2
N_TP = 2


def draw_cum_gate(key, part):
    keys = jax.random.split(jax.random.fold_in(key, 7), 5)
    fast = jax.random.randint(keys[0], (BATCH, HEADS, 1), 0, 2) == 1
    spread = jnp.exp(jax.random.uniform(keys[1], (BATCH, HEADS, 1), jnp.float32, -0.7, 0.7))
    rate = jnp.where(fast, spread / 40.0, spread / LEN)
    blocks = LEN // TOK_DEV
    factor = jnp.exp(jax.random.uniform(keys[2], (BATCH, HEADS, blocks, 1), jnp.float32, -0.85, 0.85))
    factor = jnp.broadcast_to(factor, (BATCH, HEADS, blocks, TOK_DEV)).reshape(BATCH, HEADS, LEN)
    rough = jax.random.uniform(keys[3], (BATCH, HEADS, LEN), jnp.float32, 0.5, 1.5)
    log_gate = -rate * factor * rough
    start = -jax.random.uniform(keys[4], (BATCH, HEADS, 1), jnp.float32, 0.0, 300.0)
    total = start + jnp.cumsum(log_gate, axis=-1)
    return total.reshape(BATCH, HEADS, N_TP, SPAN).astype(jnp.float32)


def steps_of(key, shape, cuts, smallest, largest):
    factor_of, own = 1.0, jax.random.fold_in(key, 6)
    for axis_at, blocks in cuts:
        steps = jnp.exp(jax.random.uniform(jax.random.fold_in(own, axis_at), (blocks,), jnp.float32, smallest / len(cuts), largest / len(cuts)))
        factor_of = factor_of * jnp.repeat(steps, shape[axis_at] // blocks).reshape([-1 if axis == axis_at else 1 for axis in range(len(shape))])
    return factor_of


def normal_values(key, shape, scale, most, pieces=(), held_as=jnp.bfloat16):
    values = jax.random.normal(key, shape, jnp.float32) * scale
    if len(pieces) > 0:
        values = steps_of(key, shape, pieces, -0.22, 0.18) * values
    return jnp.clip(values, min=-most, max=most).astype(held_as)


def setup_inputs(seed: int = 0) -> dict:
    key_of = jax.random.split(jax.random.key(seed), 6)
    tokens = normal_values(key_of[0], (BATCH, N_TP, SPAN, D), 1.0, 6.0, ((0, 2), (1, 2), (2, 8)))
    key_weight = normal_values(key_of[1], (D, HEADS * HD), D ** -0.5, 0.125)
    value_weight = normal_values(key_of[2], (D, HEADS * HD), D ** -0.5, 0.125)
    cum_gate = draw_cum_gate(jax.random.fold_in(key_of[5], 71), 0)
    query = normal_values(key_of[4], (BATCH, HEADS, HD), 3.0, 12.0, ((0, 2), (1, 8)))
    return dict(tokens=tokens, key_weight=key_weight, value_weight=value_weight, cum_gate=cum_gate, query=query)


def reference(tokens, key_weight, value_weight, cum_gate, query):
    count = tokens.shape[0]
    rows = tokens.reshape(count * LEN, D)

    def project(weight):
        out = jnp.dot(rows, weight, preferred_element_type=jnp.float32).astype(jnp.bfloat16)
        return jnp.transpose(out.reshape(count, LEN, HEADS, HD), (0, 2, 1, 3))

    keys = project(key_weight)
    values = project(value_weight)
    kv_cache = jnp.concatenate([keys, values], axis=-1)
    gate_cache = cum_gate.reshape(count, HEADS, LEN)
    scores = jnp.einsum("bhe,bhse->bhs", query.astype(jnp.float32), keys.astype(jnp.float32))
    scores = scores * (HD ** -0.5) - gate_cache
    top = jnp.max(scores, axis=-1, keepdims=True)
    weights = jnp.exp(scores - top)
    total = jnp.sum(weights, axis=-1)
    probs = weights.astype(jnp.bfloat16).astype(jnp.float32)
    weighted = jnp.einsum("bhs,bhse->bhe", probs, values.astype(jnp.float32))
    read = (weighted / total[..., None]).astype(jnp.bfloat16)
    return kv_cache, gate_cache, read
```

```python
import functools

import jax
import jax.numpy as jnp
from jax import lax
from jax.experimental import pallas as pl
from jax.experimental.pallas import tpu as pltpu
from jax.sharding import PartitionSpec as P

MESH = pl.DeviceIdType.MESH
LANES = 128


def partner(step, me, n):
    if n != 8:
        return lax.rem(me + 1 + step, n)
    plane, side = me // 2, lax.rem(me, 2)
    upper = plane // 2
    sign = 1 - 2 * upper
    inner = lax.rem(plane + upper, 2)
    turn = step // 2
    offset = jnp.where(turn == 0, 1, jnp.where(turn == 1, 2 - 3 * inner, 3 - inner))
    offset = jnp.where(turn == 3, 0, offset * sign)
    flip = lax.rem(step, 2)
    flip = jnp.where(turn == 3, 1 - flip, flip)
    return (plane + offset) * 2 + lax.rem(side + flip, 2)


def exchange_kernel(
    n, per_owner, tile, head,
    tokens, key_weight, value_weight, gates, query,
    kv, gate_in, result,
    rows, weights, outgoing, mine, theirs,
    row_sem, weight_sem, send_sem, recv_sem, gate_send, gate_recv, pair_sem,
):
    me = lax.axis_index("sp")
    core = lax.axis_index("tp")
    count = rows.shape[0]
    tiles = count // tile
    columns = weights.shape[3]
    group_heads = columns // head
    owners = group_heads // per_owner
    groups = n // owners

    def group_of(step):
        if owners == 1:
            return partner(step, me, n)
        return lax.rem(me // owners + 1 + step, groups)

    def load_rows(t):
        span = pl.ds(t * tile, tile)
        return pltpu.make_async_copy(tokens.at[span, :], rows.at[span, :], row_sem.at[t])

    def load_weight(step, which):
        at = pl.ds(pl.multiple_of(group_of(step) * columns, columns), columns)
        source = (key_weight, value_weight)[which]
        return pltpu.make_async_copy(
            source.at[:, at], weights.at[step, which], weight_sem.at[step, which]
        )

    load_rows(0).start()
    load_weight(0, 0).start()
    load_weight(0, 1).start()
    for t in range(1, tiles):
        load_rows(t).start()

    barrier = pltpu.get_barrier_semaphore()

    @pl.loop(1, n)
    def _(k):
        pl.semaphore_signal(
            barrier, inc=1, device_id={"sp": lax.rem(me + k, n)}, device_id_type=MESH
        )

    pl.semaphore_signal(barrier, inc=1, device_id={"tp": 1 - core}, device_id_type=MESH)
    pl.semaphore_wait(barrier, n)

    def gate_copy(owner):
        return pltpu.make_async_remote_copy(
            src_ref=gates.at[owner], dst_ref=gate_in.at[me],
            send_sem=gate_send.at[owner], recv_sem=gate_recv.at[me],
            device_id={"sp": owner}, device_id_type=MESH,
        )

    def gate_own():
        return pltpu.make_async_copy(gates.at[me], gate_in.at[me], gate_recv.at[me])

    @pl.loop(0, n - 1)
    def _(k):
        gate_copy(lax.rem(me + 1 + k, n)).start()

    gate_own().start()

    def block_copy(owner, t):
        return pltpu.make_async_remote_copy(
            src_ref=outgoing.at[owner, :, pl.ds(t * tile, tile), :],
            dst_ref=kv.at[:, pl.ds(pl.multiple_of(me * count + t * tile, tile), tile), :],
            send_sem=send_sem.at[owner, t], recv_sem=recv_sem.at[me, t],
            device_id={"sp": owner}, device_id_type=MESH,
        )

    def block_own(t):
        return pltpu.make_async_copy(
            outgoing.at[me, :, pl.ds(t * tile, tile), :],
            kv.at[:, pl.ds(pl.multiple_of(me * count + t * tile, tile), tile), :],
            recv_sem.at[me, t],
        )

    low = lax.broadcasted_iota(jnp.int32, (tile, LANES), 1) < head

    def project(step, first):
        group = group_of(step)

        if first:
            for ahead in range(1, min(3, groups)):
                load_weight(ahead, 0).start()
                load_weight(ahead, 1).start()
        else:
            @pl.when(step + 2 < groups)
            def _():
                load_weight(step + 2, 0).start()
                load_weight(step + 2, 1).start()

        load_weight(step, 0).wait()
        load_weight(step, 1).wait()
        for t in range(tiles):
            if first:
                load_rows(t).wait()
            left = rows[pl.ds(t * tile, tile), :]
            keys = jnp.dot(left, weights[step, 0], preferred_element_type=jnp.float32)
            values = jnp.dot(left, weights[step, 1], preferred_element_type=jnp.float32)
            for pair in range(columns // LANES):
                span = slice(pair * LANES, (pair + 1) * LANES)
                k, v = keys[:, span], values[:, span]
                joined = (
                    jnp.where(low, k, pltpu.roll(v, head, 1)),
                    jnp.where(low, pltpu.roll(k, head, 1), v),
                )
                for half in range(2):
                    local = pair * 2 + half
                    owner = group * owners + local // per_owner
                    outgoing[owner, local % per_owner, pl.ds(t * tile, tile), :] = joined[
                        half
                    ].astype(jnp.bfloat16)
            for j in range(owners):
                owner = group * owners + j

                @pl.when(owner != me)
                def _():
                    block_copy(owner, t).start()

                @pl.when(owner == me)
                def _():
                    block_own(t).start()

    project(0, True)

    def later(step, carry):
        project(step, False)
        return carry

    lax.fori_loop(1, groups, later, 0)

    wide = jnp.concatenate(
        [query[...].astype(jnp.float32), jnp.zeros((per_owner, LANES - head), jnp.float32)], axis=1
    ) * (head ** -0.5)
    head_row = lax.broadcasted_iota(jnp.int32, (per_owner, LANES), 0)
    tile_row = lax.broadcasted_iota(jnp.int32, (per_owner, tile), 0)
    queries = [jnp.where(head_row == h, wide, 0.0).astype(jnp.bfloat16) for h in range(per_owner)]

    @pl.loop(0, n - 1)
    def _(k):
        source = lax.rem(me + 1 + k, n)
        gate_copy(source).wait_send()
        pltpu.make_async_copy(gates.at[source], gate_in.at[source], gate_recv.at[source]).wait()

    gate_own().wait()

    def read_block(source, t, carry):
        top, total, weighted = carry
        span = pl.ds(pl.multiple_of(source * count + t * tile, tile), tile)
        pltpu.make_async_copy(
            outgoing.at[me, :, pl.ds(t * tile, tile), :], kv.at[:, span, :], recv_sem.at[source, t]
        ).wait()
        scores = None
        blocks = [kv[h, span, :] for h in range(per_owner)]
        for h in range(per_owner):
            term = lax.dot_general(
                queries[h], blocks[h], (((1,), (1,)), ((), ())), preferred_element_type=jnp.float32
            )
            scores = term if scores is None else scores + term
        gate = jnp.concatenate(
            [gate_in[source, h, :, pl.ds(t * tile, tile)] for h in range(per_owner)], axis=0
        )
        scores = scores - gate
        new_top = jnp.maximum(top, jnp.max(scores, axis=1, keepdims=True))
        scale = jnp.exp(top - new_top)
        probs = jnp.exp(scores - new_top)
        total = total * scale + jnp.sum(probs, axis=1, keepdims=True)
        weighted = weighted * scale
        for h in range(per_owner):
            picked = jnp.where(tile_row == h, probs, 0.0).astype(jnp.bfloat16)
            weighted = weighted + jnp.dot(picked, blocks[h], preferred_element_type=jnp.float32)
        return new_top, total, weighted

    carry = (
        jnp.full((per_owner, 1), -1e30, jnp.float32),
        jnp.zeros((per_owner, 1), jnp.float32),
        jnp.zeros((per_owner, LANES), jnp.float32),
    )

    for t in range(tiles):
        def from_source(k, carry, t=t):
            return read_block(partner(n - 1 - k, me, n), t, carry)

        carry = lax.fori_loop(0, n, from_source, carry)

    top, total, weighted = carry
    lane = lax.broadcasted_iota(jnp.int32, (per_owner, LANES), 1)
    packed = jnp.where(lane < head // 2, top, jnp.where(lane < head, total, weighted))
    mine[...] = packed
    swap = pltpu.make_async_remote_copy(
        src_ref=mine, dst_ref=theirs, send_sem=pair_sem.at[0], recv_sem=pair_sem.at[1],
        device_id={"tp": 1 - core}, device_id_type=MESH,
    )
    swap.start()

    @pl.loop(0, n - 1)
    def _(k):
        for t in range(tiles):
            block_copy(lax.rem(me + 1 + k, n), t).wait_send()

    swap.wait()
    other = theirs[...]
    one = jnp.where(core == 0, packed, other)
    two = jnp.where(core == 0, other, packed)
    top_one, top_two = one[:, :1], two[:, :1]
    joint = jnp.maximum(top_one, top_two)
    scale_one, scale_two = jnp.exp(top_one - joint), jnp.exp(top_two - joint)
    at = head // 2
    bottom = one[:, at:at + 1] * scale_one + two[:, at:at + 1] * scale_two
    result[...] = (one * scale_one + two * scale_two) / bottom


def finish_kernel(head, kv, gate_in, result, kv_out, gate_out, read, sem):
    heads, length = kv.shape[0], kv.shape[1]
    copies = [
        pltpu.make_async_copy(kv.at[h], kv_out.at[h], sem.at[h]) for h in range(heads)
    ]
    for copy in copies:
        copy.start()
    n, count = gate_in.shape[0], gate_in.shape[3]
    for source in range(n):
        gate_out[:, source * count:(source + 1) * count] = jnp.concatenate(
            [gate_in[source, h] for h in range(heads)], axis=0
        )
    read[...] = pltpu.roll(result[...], head, 1)[:, :head].astype(jnp.bfloat16)
    for copy in copies:
        copy.wait()


def on_device(n, tokens, key_weight, value_weight, cum_gate, query):
    _, _, count, width = tokens.shape
    heads = cum_gate.shape[1]
    per_owner, head = query.shape[1], query.shape[2]
    tile = 256 if count % 256 == 0 else count
    columns = max(per_owner * head, LANES)
    groups = heads * head // columns
    tiles = count // tile
    any_space = pl.BlockSpec(memory_space=pl.ANY)
    vmem = pl.BlockSpec(memory_space=pltpu.VMEM)
    kv, gate_in, result = pl.pallas_call(
        functools.partial(exchange_kernel, n, per_owner, tile, head),
        name="exchange",
        out_shape=(
            pltpu.VMEM((per_owner, n * count, 2 * head), jnp.bfloat16),
            pltpu.VMEM((n, per_owner, 1, count), jnp.float32),
            pltpu.VMEM((per_owner, 2 * head), jnp.float32),
        ),
        in_specs=[any_space] * 4 + [vmem],
        out_specs=(vmem, vmem, vmem),
        scratch_shapes=[
            pltpu.VMEM((count, width), jnp.bfloat16),
            pltpu.VMEM((groups, 2, width, columns), jnp.bfloat16),
            pltpu.VMEM((n, per_owner, count, 2 * head), jnp.bfloat16),
            pltpu.VMEM((per_owner, 2 * head), jnp.float32),
            pltpu.VMEM((per_owner, 2 * head), jnp.float32),
            pltpu.SemaphoreType.DMA((tiles,)),
            pltpu.SemaphoreType.DMA((groups, 2)),
            pltpu.SemaphoreType.DMA((n, tiles)),
            pltpu.SemaphoreType.DMA((n, tiles)),
            pltpu.SemaphoreType.DMA((n,)),
            pltpu.SemaphoreType.DMA((n,)),
            pltpu.SemaphoreType.DMA((2,)),
        ],
        compiler_params=pltpu.CompilerParams(
            collective_id=0, has_side_effects=True, vmem_limit_bytes=56 * 1024 * 1024
        ),
    )(
        tokens.reshape(count, width),
        key_weight,
        value_weight,
        cum_gate.reshape(n, per_owner, 1, count),
        query.reshape(per_owner, head),
    )
    kv_out, gate_out, read = pl.pallas_call(
        functools.partial(finish_kernel, head),
        name="finish",
        out_shape=(
            jax.ShapeDtypeStruct((per_owner, n * count, 2 * head), jnp.bfloat16),
            jax.ShapeDtypeStruct((per_owner, n * count), jnp.float32),
            jax.ShapeDtypeStruct((per_owner, head), jnp.bfloat16),
        ),
        in_specs=[vmem, vmem, vmem],
        out_specs=(any_space, vmem, vmem),
        scratch_shapes=[pltpu.SemaphoreType.DMA((per_owner,))],
        compiler_params=pltpu.CompilerParams(vmem_limit_bytes=16 * 1024 * 1024),
    )(kv, gate_in, result)
    return kv_out[None], gate_out[None], read[None]


def solution(mesh):
    placed = (P("gr", "tp", "sp", None), P(), P(), P("gr", None, "tp", "sp"), P("gr", "sp", None))
    return jax.shard_map(
        functools.partial(on_device, mesh.shape["sp"]),
        mesh=mesh,
        in_specs=placed,
        out_specs=(P("gr", "sp", "tp", None), P("gr", "sp", "tp"), P("gr", "sp", None)),
        check_vma=False,
    )
```

```python
import functools

import jax
import jax.numpy as jnp
from jax import lax
from jax.experimental import pallas as pl
from jax.experimental.pallas import tpu as pltpu
from jax.sharding import PartitionSpec as P

MESH = pl.DeviceIdType.MESH
LANES = 128


def partner(step, me, n):
    if n % 2:
        return lax.rem(me + 1 + step, n)
    turn, flip = step // 2, lax.rem(step, 2)
    flip = jnp.where(turn == n // 2 - 1, 1 - flip, flip)
    return lax.rem(me // 2 + 1 + turn, n // 2) * 2 + lax.rem(me + flip, 2)


def exchange_kernel(
    n, per_owner, tile, head,
    tokens, key_weight, value_weight, gates, query,
    kv, gate_in, result,
    rows, weights, outgoing, mine, theirs,
    row_sem, weight_sem, send_sem, recv_sem, gate_send, gate_recv, pair_sem,
):
    me = lax.axis_index("sp")
    core = lax.axis_index("tp")
    count = rows.shape[0]
    tiles = count // tile
    columns = weights.shape[3]
    group_heads = columns // head
    owners = group_heads // per_owner
    groups = n // owners

    def group_of(step):
        if owners == 1:
            return partner(step, me, n)
        return lax.rem(me // owners + 1 + step, groups)

    def load_rows(t):
        span = pl.ds(t * tile, tile)
        return pltpu.make_async_copy(tokens.at[span, :], rows.at[span, :], row_sem.at[t])

    def load_weight(step, which):
        at = pl.ds(pl.multiple_of(group_of(step) * columns, columns), columns)
        source = (key_weight, value_weight)[which]
        return pltpu.make_async_copy(
            source.at[:, at], weights.at[step, which], weight_sem.at[step, which]
        )

    load_rows(0).start()
    load_weight(0, 0).start()
    load_weight(0, 1).start()
    for t in range(1, tiles):
        load_rows(t).start()

    barrier = pltpu.get_barrier_semaphore()

    @pl.loop(1, n)
    def _(k):
        pl.semaphore_signal(
            barrier, inc=1, device_id={"sp": lax.rem(me + k, n)}, device_id_type=MESH
        )

    pl.semaphore_signal(barrier, inc=1, device_id={"tp": 1 - core}, device_id_type=MESH)
    pl.semaphore_wait(barrier, n)

    def gate_copy(owner):
        return pltpu.make_async_remote_copy(
            src_ref=gates.at[owner], dst_ref=gate_in.at[me],
            send_sem=gate_send.at[owner], recv_sem=gate_recv.at[me],
            device_id={"sp": owner}, device_id_type=MESH,
        )

    def gate_own():
        return pltpu.make_async_copy(gates.at[me], gate_in.at[me], gate_recv.at[me])

    @pl.loop(0, n - 1)
    def _(k):
        gate_copy(lax.rem(me + 1 + k, n)).start()

    gate_own().start()

    def block_copy(owner, t):
        return pltpu.make_async_remote_copy(
            src_ref=outgoing.at[owner, :, pl.ds(t * tile, tile), :],
            dst_ref=kv.at[:, pl.ds(pl.multiple_of(me * count + t * tile, tile), tile), :],
            send_sem=send_sem.at[owner, t], recv_sem=recv_sem.at[me, t],
            device_id={"sp": owner}, device_id_type=MESH,
        )

    def block_own(t):
        return pltpu.make_async_copy(
            outgoing.at[me, :, pl.ds(t * tile, tile), :],
            kv.at[:, pl.ds(pl.multiple_of(me * count + t * tile, tile), tile), :],
            recv_sem.at[me, t],
        )

    low = lax.broadcasted_iota(jnp.int32, (tile, LANES), 1) < head

    def project(step, first):
        group = group_of(step)

        if first:
            for ahead in range(1, min(3, groups)):
                load_weight(ahead, 0).start()
                load_weight(ahead, 1).start()
        else:
            @pl.when(step + 2 < groups)
            def _():
                load_weight(step + 2, 0).start()
                load_weight(step + 2, 1).start()

        load_weight(step, 0).wait()
        load_weight(step, 1).wait()
        for t in range(tiles):
            if first:
                load_rows(t).wait()
            left = rows[pl.ds(t * tile, tile), :]
            keys = jnp.dot(left, weights[step, 0], preferred_element_type=jnp.float32)
            values = jnp.dot(left, weights[step, 1], preferred_element_type=jnp.float32)
            for pair in range(columns // LANES):
                span = slice(pair * LANES, (pair + 1) * LANES)
                k, v = keys[:, span], values[:, span]
                joined = (
                    jnp.where(low, k, pltpu.roll(v, head, 1)),
                    jnp.where(low, pltpu.roll(k, head, 1), v),
                )
                for half in range(2):
                    local = pair * 2 + half
                    owner = group * owners + local // per_owner
                    outgoing[owner, local % per_owner, pl.ds(t * tile, tile), :] = joined[
                        half
                    ].astype(jnp.bfloat16)
            for j in range(owners):
                owner = group * owners + j

                @pl.when(owner != me)
                def _():
                    block_copy(owner, t).start()

                @pl.when(owner == me)
                def _():
                    block_own(t).start()

    project(0, True)

    def later(step, carry):
        project(step, False)
        return carry

    lax.fori_loop(1, groups, later, 0)

    wide = jnp.concatenate(
        [query[...].astype(jnp.float32), jnp.zeros((per_owner, LANES - head), jnp.float32)], axis=1
    ) * (head ** -0.5)
    head_row = lax.broadcasted_iota(jnp.int32, (per_owner, LANES), 0)
    tile_row = lax.broadcasted_iota(jnp.int32, (per_owner, tile), 0)
    queries = [jnp.where(head_row == h, wide, 0.0).astype(jnp.bfloat16) for h in range(per_owner)]

    @pl.loop(0, n - 1)
    def _(k):
        source = lax.rem(me + 1 + k, n)
        gate_copy(source).wait_send()
        pltpu.make_async_copy(gates.at[source], gate_in.at[source], gate_recv.at[source]).wait()

    gate_own().wait()

    def read_block(source, t, carry):
        top, total, weighted = carry
        span = pl.ds(pl.multiple_of(source * count + t * tile, tile), tile)
        pltpu.make_async_copy(
            outgoing.at[me, :, pl.ds(t * tile, tile), :], kv.at[:, span, :], recv_sem.at[source, t]
        ).wait()
        scores = None
        blocks = [kv[h, span, :] for h in range(per_owner)]
        for h in range(per_owner):
            term = lax.dot_general(
                queries[h], blocks[h], (((1,), (1,)), ((), ())), preferred_element_type=jnp.float32
            )
            scores = term if scores is None else scores + term
        gate = jnp.concatenate(
            [gate_in[source, h, :, pl.ds(t * tile, tile)] for h in range(per_owner)], axis=0
        )
        scores = scores - gate
        new_top = jnp.maximum(top, jnp.max(scores, axis=1, keepdims=True))
        scale = jnp.exp(top - new_top)
        probs = jnp.exp(scores - new_top)
        total = total * scale + jnp.sum(probs, axis=1, keepdims=True)
        weighted = weighted * scale
        for h in range(per_owner):
            picked = jnp.where(tile_row == h, probs, 0.0).astype(jnp.bfloat16)
            weighted = weighted + jnp.dot(picked, blocks[h], preferred_element_type=jnp.float32)
        return new_top, total, weighted

    carry = (
        jnp.full((per_owner, 1), -1e30, jnp.float32),
        jnp.zeros((per_owner, 1), jnp.float32),
        jnp.zeros((per_owner, LANES), jnp.float32),
    )

    for t in range(tiles):
        def from_source(k, carry, t=t):
            return read_block(partner(n - 1 - k, me, n), t, carry)

        carry = lax.fori_loop(0, n, from_source, carry)

    top, total, weighted = carry
    lane = lax.broadcasted_iota(jnp.int32, (per_owner, LANES), 1)
    packed = jnp.where(lane < head // 2, top, jnp.where(lane < head, total, weighted))
    mine[...] = packed
    swap = pltpu.make_async_remote_copy(
        src_ref=mine, dst_ref=theirs, send_sem=pair_sem.at[0], recv_sem=pair_sem.at[1],
        device_id={"tp": 1 - core}, device_id_type=MESH,
    )
    swap.start()

    @pl.loop(0, n - 1)
    def _(k):
        for t in range(tiles):
            block_copy(lax.rem(me + 1 + k, n), t).wait_send()

    swap.wait()
    other = theirs[...]
    one = jnp.where(core == 0, packed, other)
    two = jnp.where(core == 0, other, packed)
    top_one, top_two = one[:, :1], two[:, :1]
    joint = jnp.maximum(top_one, top_two)
    scale_one, scale_two = jnp.exp(top_one - joint), jnp.exp(top_two - joint)
    at = head // 2
    bottom = one[:, at:at + 1] * scale_one + two[:, at:at + 1] * scale_two
    result[...] = (one * scale_one + two * scale_two) / bottom


def finish_kernel(head, kv, gate_in, result, kv_out, gate_out, read, sem):
    heads, length = kv.shape[0], kv.shape[1]
    copies = [
        pltpu.make_async_copy(kv.at[h], kv_out.at[h], sem.at[h]) for h in range(heads)
    ]
    for copy in copies:
        copy.start()
    n, count = gate_in.shape[0], gate_in.shape[3]
    for source in range(n):
        gate_out[:, source * count:(source + 1) * count] = jnp.concatenate(
            [gate_in[source, h] for h in range(heads)], axis=0
        )
    read[...] = pltpu.roll(result[...], head, 1)[:, :head].astype(jnp.bfloat16)
    for copy in copies:
        copy.wait()


def on_device(n, tokens, key_weight, value_weight, cum_gate, query):
    _, _, count, width = tokens.shape
    heads = cum_gate.shape[1]
    per_owner, head = query.shape[1], query.shape[2]
    tile = 256 if count % 256 == 0 else count
    columns = max(per_owner * head, LANES)
    groups = heads * head // columns
    tiles = count // tile
    any_space = pl.BlockSpec(memory_space=pl.ANY)
    vmem = pl.BlockSpec(memory_space=pltpu.VMEM)
    kv, gate_in, result = pl.pallas_call(
        functools.partial(exchange_kernel, n, per_owner, tile, head),
        name="exchange",
        out_shape=(
            pltpu.VMEM((per_owner, n * count, 2 * head), jnp.bfloat16),
            pltpu.VMEM((n, per_owner, 1, count), jnp.float32),
            pltpu.VMEM((per_owner, 2 * head), jnp.float32),
        ),
        in_specs=[any_space] * 4 + [vmem],
        out_specs=(vmem, vmem, vmem),
        scratch_shapes=[
            pltpu.VMEM((count, width), jnp.bfloat16),
            pltpu.VMEM((groups, 2, width, columns), jnp.bfloat16),
            pltpu.VMEM((n, per_owner, count, 2 * head), jnp.bfloat16),
            pltpu.VMEM((per_owner, 2 * head), jnp.float32),
            pltpu.VMEM((per_owner, 2 * head), jnp.float32),
            pltpu.SemaphoreType.DMA((tiles,)),
            pltpu.SemaphoreType.DMA((groups, 2)),
            pltpu.SemaphoreType.DMA((n, tiles)),
            pltpu.SemaphoreType.DMA((n, tiles)),
            pltpu.SemaphoreType.DMA((n,)),
            pltpu.SemaphoreType.DMA((n,)),
            pltpu.SemaphoreType.DMA((2,)),
        ],
        compiler_params=pltpu.CompilerParams(
            collective_id=0, has_side_effects=True, vmem_limit_bytes=56 * 1024 * 1024
        ),
    )(
        tokens.reshape(count, width),
        key_weight,
        value_weight,
        cum_gate.reshape(n, per_owner, 1, count),
        query.reshape(per_owner, head),
    )
    kv_out, gate_out, read = pl.pallas_call(
        functools.partial(finish_kernel, head),
        name="finish",
        out_shape=(
            jax.ShapeDtypeStruct((per_owner, n * count, 2 * head), jnp.bfloat16),
            jax.ShapeDtypeStruct((per_owner, n * count), jnp.float32),
            jax.ShapeDtypeStruct((per_owner, head), jnp.bfloat16),
        ),
        in_specs=[vmem, vmem, vmem],
        out_specs=(any_space, vmem, vmem),
        scratch_shapes=[pltpu.SemaphoreType.DMA((per_owner,))],
        compiler_params=pltpu.CompilerParams(vmem_limit_bytes=16 * 1024 * 1024),
    )(kv, gate_in, result)
    return kv_out[None], gate_out[None], read[None]


def solution(mesh):
    placed = (P("gr", "tp", "sp", None), P(), P(), P("gr", None, "tp", "sp"), P("gr", "sp", None))
    return jax.shard_map(
        functools.partial(on_device, mesh.shape["sp"]),
        mesh=mesh,
        in_specs=placed,
        out_specs=(P("gr", "sp", "tp", None), P("gr", "sp", "tp"), P("gr", "sp", None)),
        check_vma=False,
    )
```
